32 devices in a mesh: grp: 2 (over y), ep: 4 (over z), tp: 4 (over x, core).
Axes of the slice: x: 2, y: 2, z: 4, core: 2. Of those that a mesh axis runs over, the one named last changes fastest.
Arguments:
- tokens: bfloat16 [2048, 2048], P(('grp', 'ep')), parts along dimension 0, may hold values from -6 to 6
- in_gain: bfloat16 [2048], replicated, may hold values from 0.099609375 to 1.8984375
- expert_ids: int32 [2048, 2], P(('grp', 'ep')), parts along dimension 0, may hold values from 0 to 3, all different within a row; in each aligned block of 256 rows (0 to 255, 256 to 511, ...) at most 256 rows name the same one
- route_weights: float32 [2048, 2], P(('grp', 'ep')), parts along dimension 0, may hold values from 0.1 to 1
- gate_weight: bfloat16 [4, 2048, 2048], P('ep', None, 'tp'), may hold values from -0.375 to 0.375
- up_weight: bfloat16 [4, 2048, 2048], P('ep', None, 'tp'), may hold values from -0.375 to 0.375
- down_weight: bfloat16 [4, 2048, 2048], P('ep', 'tp')
- out_gain: bfloat16 [2048], P('tp'), may hold values from 0.099609375 to 1.8984375
Outputs:
- normed_out: bfloat16 [2048, 2048], P(('grp', 'ep'), 'tp'), parts along dimension 0
The draws below stay inside these ranges and needn't reach their ends.
There are 2 independent parts, one for each index of `grp`. The reference program is written for one: setup_inputs(seed, part) draws one part's arguments, and reference() takes and returns one part's arrays. A program takes and returns all parts, laid end to end along the dimension named above; an argument that names none is the same for every part. Nothing has to cross between parts.
Inputs may be any that keep to these rules, and one draw needn't show every extreme that they name: `expert_ids`: each row names 2 different experts. Among the 256 rows of one index of ep, no expert is named more than 256 times, a bound that some block reaches.
All inputs are finite; a program needn't handle non-finite values.
Results may differ from the reference program's by a relative error of at most 0.015.
Values may be sent and summed in bfloat16 or wider, within the bound.
A program may use at most 64 MiB of HBM per device.

```python
import math
import jax
import jax.numpy as jnp
import numpy as np
from jax import lax

D = 2048
FF = 2048
TOP_K = 2
TOK_DEV = 256
EXPERTS = 4
TOKENS = 1024
CAP = 256
N_EP = 4
N_TP = 4


def draw_down_weight(key, part):
    column = jnp.arange(D, dtype=jnp.float32) / D
    entries = jax.random.normal(key, (EXPERTS, FF, D), jnp.float32)
    scales = jnp.exp(jnp.log(4.0) * column)
    return (entries * scales[None, None, :] * FF ** (-0.5)).astype(jnp.bfloat16)


def level_of(stream_key, dims, shards, least, high):
    def one(position, shards_of):
        heights = jax.random.uniform(jax.random.fold_in(jax.random.fold_in(stream_key, 6), position), (shards_of,), jnp.float32, least / len(shards), high / len(shards))
        return jnp.repeat(jnp.exp(heights), dims[position] // shards_of).reshape((-1,) + (1,) * (len(dims) - position - 1))

    loudness = one(*shards[0])
    for cut in shards[1:]:
        loudness = loudness * one(*cut)
    return loudness


def routed_block(rng, own, number, rows, number_of, top, bound, slope):
    sequence = jax.random.permutation(rng, number_of)
    heavy_load, common = shares(number_of, rows * top, bound, slope, True), shares(number_of, rows * top, bound, slope, False)
    places = jnp.arange(number_of)

    def named(lengths, offset_by):
        used = int((lengths > 0).sum())
        fixed = max(1, used // 4)
        moved = fixed + (places - fixed + offset_by * (used - fixed)) % max(1, number_of - fixed)
        return jnp.zeros((number_of,), jnp.int32).at[sequence[jnp.where(places < fixed, places, moved)]].set(jnp.asarray(lengths, jnp.int32))

    lengths = jnp.where(number % 4 == 0, named(heavy_load, number // 4), named(common, number - number // 4 - 1))
    mixed = jax.random.permutation(jax.random.fold_in(own, 3), number_of)
    giver, taker = mixed[0:number_of // 2 * 2:2], mixed[1:number_of // 2 * 2:2]
    margin = jnp.minimum(lengths[giver] - 1, bound - lengths[taker]) // 2
    margin = jnp.where((giver == sequence[0]) | (taker == sequence[0]) | (lengths[taker] == 0), 0, jnp.maximum(margin, 0))
    moved = jax.random.randint(jax.random.fold_in(own, 4), (number_of // 2,), 0, 1 << 20) % (margin + 1)
    lengths = lengths.at[giver].add(-moved).at[taker].add(moved)
    items = jnp.searchsorted(jnp.cumsum(lengths), jnp.arange(rows * top), side="right").astype(jnp.int32)
    listing = items.reshape(top, rows).T
    listing = listing[jax.random.permutation(jax.random.fold_in(own, 1), rows)]
    offset_by = jax.random.randint(jax.random.fold_in(own, 2), (rows, 1), 0, top)
    return jnp.take_along_axis(listing, (jnp.arange(top)[None, :] + offset_by) % top, axis=1)


def shares(number_of, total, limit, lean, full):
    weights = [(1 << 20) // math.isqrt(grade ** lean) + 1 for grade in range(1, number_of + 1)]
    largest = limit if full else min(limit, max(-(-total // number_of), total * weights[0] // sum(weights)))
    least = 1 if total - largest >= number_of - 1 else 0
    given, surplus = [largest] + [least] * (number_of - 1), total - largest - least * (number_of - 1)
    while surplus > 0:
        free = [i for i in range(1, number_of) if given[i] < largest] or [i for i in range(1, number_of) if given[i] < limit]
        mass, left = sum([weights[i] for i in free]), surplus
        for i in free:
            addition = min(limit - given[i], max(1, left * weights[i] // mass), surplus)
            given[i] = given[i] + addition
            surplus = surplus - addition
    return np.array(given)


def centred(key, extent, spread, limit, cuts=(), kind=jnp.bfloat16):
    loudness = level_of(key, extent, cuts, -0.22, 0.18) if cuts else 1.0
    array = jax.random.normal(key, extent, jnp.float32) * spread * loudness
    return jnp.minimum(jnp.maximum(array, -limit), limit).astype(kind)


def setup_inputs(seed: int = 0, part: int = 0) -> dict:
    keys = jax.random.split(jax.random.key(seed), 9)
    part_splits = jax.random.split(jax.random.fold_in(keys[8], part), 9)
    tokens = centred(part_splits[0], (TOKENS, D), 1.0, 6.0, ((0, 4),))
    in_gain = jnp.clip(1.0 + 0.18 * jax.random.normal(keys[1], (D,), jnp.float32), 0.099609375, 1.8984375).astype(jnp.bfloat16)
    expert_ids_keys = jax.random.split(jax.random.fold_in(part_splits[2], 1), TOKENS // TOK_DEV)
    expert_ids_turns = jax.random.permutation(jax.random.fold_in(part_splits[2], 3), TOKENS // TOK_DEV)
    expert_ids = jax.vmap(lambda own, number: routed_block(jax.random.fold_in(part_splits[2], 2), own, number, TOK_DEV, EXPERTS, TOP_K, CAP, 2))(expert_ids_keys, expert_ids_turns).reshape((TOKENS, TOP_K))
    route_weights = jnp.clip(jnp.exp(math.log(1.0) - 2.3025851 * jax.random.uniform(part_splits[3], (TOKENS, TOP_K), jnp.float32) ** level_of(part_splits[3], (TOKENS, TOP_K), ((0, 4),), -0.2, 0.2)), 0.1, 1.0)
    gate_weight = centred(keys[4], (EXPERTS, D, FF), (D // 8) ** -0.5, 0.375, ((0, 4), (2, 4)))
    up_weight = centred(keys[5], (EXPERTS, D, FF), (D // 8) ** -0.5, 0.375, ((0, 4), (2, 4)))
    down_weight = draw_down_weight(jax.random.fold_in(keys[8], 71), part)
    out_gain = jnp.clip(1.0 + 0.18 * jax.random.normal(keys[7], (D,), jnp.float32), 0.099609375, 1.8984375).astype(jnp.bfloat16)
    return dict(tokens=tokens, in_gain=in_gain, expert_ids=expert_ids, route_weights=route_weights, gate_weight=gate_weight, up_weight=up_weight, down_weight=down_weight, out_gain=out_gain)


eps = 1e-05

def reference(tokens, in_gain, expert_ids, route_weights, gate_weight, up_weight, down_weight, out_gain):
    xf = tokens.astype(jnp.float32)
    normed_in = (xf * lax.rsqrt(lax.optimization_barrier(jnp.mean(xf * xf, axis=1, keepdims=True)) + eps) * in_gain.astype(jnp.float32)).astype(jnp.bfloat16)
    ids = expert_ids.reshape(N_EP, TOK_DEV * TOP_K)
    onehot = (ids[:, :, None] == jnp.arange(EXPERTS, dtype=jnp.int32)[None, None, :]).astype(jnp.int32)
    earlier = jnp.cumsum(onehot, axis=1) - onehot
    slot = lax.optimization_barrier(jnp.sum(earlier * onehot, axis=2))
    block = jnp.arange(N_EP, dtype=jnp.int32)[:, None]
    row_of = ((ids * N_EP + block) * CAP + slot).reshape(-1).astype(jnp.int32)
    token_of = (jnp.arange(TOKENS * TOP_K, dtype=jnp.int32) // TOP_K).astype(jnp.int32)
    row_token = jnp.full((EXPERTS * N_EP * CAP,), TOKENS, jnp.int32).at[row_of].set(token_of)
    row_token = row_token.reshape(EXPERTS, N_EP * CAP)
    extended = jnp.concatenate([normed_in, jnp.zeros((1, D), jnp.bfloat16)], axis=0)

    def expert_rows(args):
        picks, w_gate, w_up, w_down = args
        rows = extended[picks]
        gate_pre = jnp.dot(rows, w_gate, preferred_element_type=jnp.float32)
        up_pre = jnp.dot(rows, w_up, preferred_element_type=jnp.float32)
        g = jnp.minimum(gate_pre, 7.0)
        u = jnp.clip(up_pre, -7.0, 7.0)
        act = (g * jax.nn.sigmoid(1.702 * g) * (u + 1.0)).astype(jnp.bfloat16)
        groups = act.reshape(N_EP * CAP, N_TP, FF // N_TP).astype(jnp.float32)
        wd = w_down.reshape(N_TP, FF // N_TP, D).astype(jnp.float32)
        partial_value = jnp.einsum('rgf,gfd->grd', groups, wd).astype(jnp.bfloat16)
        return lax.optimization_barrier(jnp.sum(partial_value.astype(jnp.float32), axis=0)).astype(jnp.bfloat16)
    expert_out = lax.map(expert_rows, (row_token, gate_weight, up_weight, down_weight))
    expert_out = expert_out.reshape(EXPERTS * N_EP * CAP, D)
    picked = expert_out[row_of].astype(jnp.float32).reshape(TOKENS, TOP_K, D)
    combined = lax.optimization_barrier(jnp.sum(picked * route_weights[:, :, None], axis=1))
    scale = lax.rsqrt(lax.optimization_barrier(jnp.mean(combined * combined, axis=1, keepdims=True)) + eps)
    return (combined * scale * out_gain.astype(jnp.float32)).astype(jnp.bfloat16)
```

```python
import jax
import jax.numpy as jnp
from jax import lax
from jax.experimental import pallas as pl
from jax.experimental.pallas import tpu as pltpu
from jax.sharding import PartitionSpec as P

eps = 1e-05
f32 = jnp.float32
bf16 = jnp.bfloat16
pieces = 2
lanes = 128

whole_in = (1, )
whole_out = (0, 1, )

send_order = (
    (
        (2, 0), (3, 0), (1, 0), (1, 1), (2, 1), (3, 1),
    ),
    (
        (2, 0), (1, 0), (3, 0), (1, 1), (3, 1), (2, 1),
    ),
)

schedule = (
    ("C", 0, 1), ("Z", 3, 0), ("C", 0, 0), ("Z", 1, 0), ("X", 3, 0), ("C", 3, 0),
    ("Z", 2, 0), ("P", 3, 0), ("X", 1, 0), ("C", 1, 0), ("Z", 1, 1), ("X", 2, 0),
    ("Z", 3, 1), ("P", 1, 0), ("X", 1, 1), ("C", 2, 0), ("P", 2, 0), ("Q", 3, 0),
    ("C", 1, 1), ("Z", 2, 1), ("Q", 1, 0), ("X", 3, 1), ("C", 3, 1), ("Q", 2, 0),
    ("P", 3, 1), ("X", 2, 1), ("C", 2, 1), ("P", 1, 1), ("P", 2, 1), ("Q", 3, 1),
    ("P", 0, 1), ("Q", 1, 1), ("P", 0, 0), ("Q", 2, 1), ("Q", 0, 1), ("Q", 0, 0),
)


def layer_kernel(
    tok, gain, ids, rw, wg, wu, wd, og, out,
    raw, xbuf, wgb, wub, wdb, g32, share, part, drecv, esend, erecv, brecv, fin, ret, acc, sq,
    ts, ws, zs, zr, bs, br, ys, yr, xs, xr, ps, pr, ds, dr, es, er, fs, fr, qs, qr,
):
    z, p = lax.axis_index("ep"), lax.axis_index("tp")
    n_ep, n_q, rows, fb = xbuf.shape
    part_rows = rows // pieces
    half, c = p // 2, p % 2
    mate = half * 2 + 1 - c
    across = (1 - half) * 2 + c
    diagonal = (1 - half) * 2 + 1 - c
    hi = z // 2
    order = (z, 1 - z + hi * 4, 2 - hi, 3 - 3 * hi)
    middle = jnp.logical_or(z == 1, z == 2)

    def span(h):
        return pl.ds(h * part_rows, part_rows)

    def remote(src, dst, s, r, **where):
        return pltpu.make_async_remote_copy(
            src_ref=src, dst_ref=dst, send_sem=s, recv_sem=r,
            device_id=where, device_id_type=pl.DeviceIdType.MESH,
        )

    def signal(**where):
        pl.semaphore_signal(barrier, inc=1, device_id=where, device_id_type=pl.DeviceIdType.MESH)

    loads = [
        [
            pltpu.make_async_copy(
                tok.at[span(h), pl.ds(q * fb, fb)], raw.at[q, span(h)], ts.at[h, q]
            )
            for q in range(n_q)
        ]
        for h in range(pieces)
    ]
    weights = [
        pltpu.make_async_copy(wg.at[0], wgb, ws.at[0]),
        pltpu.make_async_copy(wu.at[0], wub, ws.at[1]),
    ] + [
        pltpu.make_async_copy(wd.at[0, :, pl.ds(q * fb, fb)], wdb.at[q], ws.at[2 + q])
        for q in range(n_q)
    ]
    barrier = pltpu.get_barrier_semaphore()
    for peer in (mate, across, diagonal):
        signal(tp=peer)
    for b in order[1:]:
        signal(ep=b)
    for copy in sum(loads, []) + weights:
        copy.start()
    for q in range(n_q):
        g32[q] = gain[q * (fb // lanes):(q + 1) * (fb // lanes), :].astype(f32)
    share[...] = jnp.transpose(jnp.concatenate(
        [
            sum(jnp.where(ids[k:k + 1, :] == e, rw[k:k + 1, :], 0.0) for k in range(ids.shape[0]))
            for e in order
        ]
        + [jnp.zeros((lanes - len(order), rows), f32)],
        axis=0,
    ))

    sends = []

    def push(copy):
        copy.start()
        sends.append(copy)

    def scaled(value, i, r):
        w = share[r, i:i + 1]
        return jnp.where(w != 0.0, value * w, 0.0)

    def normalize(h):
        for copy in loads[h]:
            copy.wait()
        total = jnp.zeros((part_rows, 1), f32)
        for q in range(n_q):
            v = raw[q, span(h)].astype(f32)
            total += jnp.sum(v * v, axis=1, keepdims=True)
        scale = lax.rsqrt(total / (n_q * fb) + eps)

        def one(q):
            for j in range(fb // lanes):
                cols = slice(j * lanes, (j + 1) * lanes)
                g = g32[q][j:j + 1, :]
                xbuf[z, q, span(h), cols] = (
                    raw[q, span(h), cols].astype(f32) * scale * g
                ).astype(bf16)

        one(p)
        if h in whole_in:
            one(across)
        if h == 0:
            pl.semaphore_wait(barrier, 6)
        mine, other = xbuf.at[z, p, span(h)], xbuf.at[z, across, span(h)]
        first = {
            i: [remote(mine, mine, zs.at[i, h], zr.at[z, h], ep=order[i])] for i in (1, 2, 3)
        }
        if h in whole_in:
            first[1].append(remote(other, other, ys.at[h], yr.at[h], ep=order[1]))
        ends, middles = (tuple(i for i, k in o if k == h) for o in send_order)

        def start(places):
            for i in places:
                for copy in first[i]:
                    copy.start()

        if ends == middles:
            start(ends)
        else:
            pl.when(middle)(lambda: start(middles))
            pl.when(jnp.logical_not(middle))(lambda: start(ends))
        sends.extend(sum(first.values(), []))
        for q in (mate, diagonal) if h in whole_in else (across, mate, diagonal):
            one(q)

    def arrived(ref, sem):
        pltpu.make_async_copy(ref, ref, sem).wait()

    def stage_z(i, h):
        b = order[i]
        piece = xbuf.at[b, p, span(h)]
        arrived(piece, zr.at[b, h])
        if i > 1 or h not in whole_in:
            push(remote(piece, piece, xs.at[b, h], xr.at[b, h], tp=across))
        push(remote(piece, piece, ps.at[0, b, h], pr.at[0, b, h], tp=mate))

    def stage_x(i, h):
        b = order[i]
        piece = xbuf.at[b, across, span(h)]
        arrived(piece, yr.at[h] if i == 1 and h in whole_in else xr.at[b, h])
        push(remote(piece, piece, ps.at[1, b, h], pr.at[1, b, h], tp=mate))

    def stage_c(i, h):
        b = order[i]
        if i > 0:
            arrived(xbuf.at[b, mate, span(h)], pr.at[0, b, h])
            arrived(xbuf.at[b, diagonal, span(h)], pr.at[1, b, h])
        elif (i, h) == own_first:
            for copy in weights:
                copy.wait()
        x = jnp.concatenate([xbuf[b, q, span(h)] for q in range(n_q)], axis=1)
        gate = jnp.minimum(jnp.dot(x, wgb[...], preferred_element_type=f32), 7.0)
        up = jnp.clip(jnp.dot(x, wub[...], preferred_element_type=f32), -7.0, 7.0)
        act = (gate * jax.nn.sigmoid(1.702 * gate) * (up + 1.0)).astype(bf16)

        def down(q):
            part[b, q, span(h)] = jnp.dot(
                act, wdb[q], preferred_element_type=f32
            ).astype(bf16)

        for s in range(2):
            q = 2 * s + 1 - c
            down(q)
            push(remote(
                part.at[b, q, span(h)], drecv.at[b, s, span(h)],
                ds.at[b, s, h], dr.at[b, s, h], tp=mate,
            ))
        for s in range(2):
            down(2 * s + c)

    def stage_p(i, h):
        b, r = order[i], span(h)
        arrived(drecv.at[b, 1 - half, r], dr.at[b, 1 - half, h])
        value = part[b, across, r].astype(f32) + drecv[b, 1 - half, r].astype(f32)
        if i == 0:
            value = scaled(value, 0, r)
            if h in whole_out:
                arrived(brecv.at[r], br.at[h])
                value += scaled(brecv[r].astype(f32), 1, r)
        esend[b, r] = value.astype(bf16)
        if i == 1 and h in whole_out:
            push(remote(esend.at[b, r], brecv.at[r], bs.at[h], br.at[h], ep=b))
        else:
            push(remote(esend.at[b, r], erecv.at[b, r], es.at[b, h], er.at[b, h], tp=across))

    def stage_q(i, h):
        b, r = order[i], span(h)
        arrived(drecv.at[b, half, r], dr.at[b, half, h])
        value = part[b, p, r].astype(f32) + drecv[b, half, r].astype(f32)
        if i == 0:
            value = scaled(value, 0, r)
        if i != 1 or h not in whole_out:
            arrived(erecv.at[b, r], er.at[b, h])
            value += erecv[b, r].astype(f32)
        if i == 0:
            acc[r] = value
        else:
            fin[b, r] = value.astype(bf16)
            push(remote(fin.at[b, r], ret.at[z, r], fs.at[b, h], fr.at[z, h], ep=b))

    for h in range(pieces):
        with jax.named_scope(f"N{h}"):
            normalize(h)
    own_first = next(s[1:] for s in schedule if s[0] == "C")
    stages = {"Z": stage_z, "X": stage_x, "C": stage_c, "P": stage_p, "Q": stage_q}
    for name, i, h in schedule:
        with jax.named_scope(f"{name}{i}{h}"):
            stages[name](i, h)

    with jax.named_scope("comb"):
        sums = []
        for h in range(pieces):
            r = span(h)
            combined = acc[r]
            for i in (1, 2, 3):
                arrived(ret.at[order[i], r], fr.at[order[i], h])
                combined += scaled(ret[order[i], r].astype(f32), i, r)
            acc[r] = combined
            sums.append(jnp.sum(combined * combined, axis=1, keepdims=True))
        sums = jnp.concatenate(sums, axis=0)
        sq[p] = jnp.transpose(jnp.broadcast_to(sums, (rows, lanes)))[:8]
    for peer, k in ((mate, 0), (across, 1), (diagonal, 2)):
        push(remote(sq.at[p], sq.at[p], qs.at[k], qr.at[p], tp=peer))
    with jax.named_scope("sqw"):
        for peer in (mate, across, diagonal):
            arrived(sq.at[peer], qr.at[peer])
    with jax.named_scope("out"):
        squares = jnp.transpose(sq[0] + sq[1] + sq[2] + sq[3])[:, :1]
        scale = lax.rsqrt(squares / (n_q * fb) + eps)
        og32 = og[...].astype(f32)
        for j in range(fb // lanes):
            cols = slice(j * lanes, (j + 1) * lanes)
            out[:, cols] = (acc[:, cols] * scale * og32[j:j + 1, :]).astype(bf16)
    for copy in sends:
        copy.wait_send()


def fused(tokens, in_gain, expert_ids, route_weights, gate_weight, up_weight, down_weight, out_gain):
    n_ep, n_tp = lax.axis_size("ep"), lax.axis_size("tp")
    rows, width = tokens.shape
    hidden = gate_weight.shape[2]
    fb = width // n_tp
    vmem = pl.BlockSpec(memory_space=pltpu.VMEM)
    hbm = pl.BlockSpec(memory_space=pl.ANY)
    sem = pltpu.SemaphoreType.DMA
    piece = (rows, fb)
    return pl.pallas_call(
        layer_kernel,
        out_shape=jax.ShapeDtypeStruct(piece, bf16),
        in_specs=[hbm, vmem, vmem, vmem, hbm, hbm, hbm, vmem],
        out_specs=vmem,
        scratch_shapes=[
            pltpu.VMEM((n_tp,) + piece, bf16),
            pltpu.VMEM((n_ep, n_tp) + piece, bf16),
            pltpu.VMEM((width, hidden), bf16),
            pltpu.VMEM((width, hidden), bf16),
            pltpu.VMEM((n_tp, hidden, fb), bf16),
            pltpu.VMEM((n_tp, fb // lanes, lanes), f32),
            pltpu.VMEM((rows, lanes), f32),
            pltpu.VMEM((n_ep, n_tp) + piece, bf16),
            pltpu.VMEM((n_ep, 2) + piece, bf16),
            pltpu.VMEM((n_ep,) + piece, bf16),
            pltpu.VMEM((n_ep,) + piece, bf16),
            pltpu.VMEM(piece, bf16),
            pltpu.VMEM((n_ep,) + piece, bf16),
            pltpu.VMEM((n_ep,) + piece, bf16),
            pltpu.VMEM(piece, f32),
            pltpu.VMEM((n_tp, 8, rows), f32),
            sem((pieces, n_tp)), sem((2 + n_tp,)),
            sem((4, pieces)), sem((n_ep, pieces)),
            sem((pieces,)), sem((pieces,)),
            sem((pieces,)), sem((pieces,)),
            sem((n_ep, pieces)), sem((n_ep, pieces)),
            sem((2, n_ep, pieces)), sem((2, n_ep, pieces)),
            sem((n_ep, 2, pieces)), sem((n_ep, 2, pieces)),
            sem((n_ep, pieces)), sem((n_ep, pieces)),
            sem((n_ep, pieces)), sem((n_ep, pieces)),
            sem((3,)), sem((n_tp,)),
        ],
        compiler_params=pltpu.CompilerParams(
            collective_id=0, has_side_effects=True, vmem_limit_bytes=60 * 1024 * 1024
        ),
        name="layer",
    )(
        tokens, in_gain.reshape(-1, lanes), expert_ids.T, route_weights.T,
        gate_weight, up_weight, down_weight, out_gain.reshape(-1, lanes),
    )


def on_device(
    tokens, in_gain, expert_ids, route_weights, gate_weight, up_weight, down_weight, out_gain
):
    n_ep = lax.axis_size("ep")
    n_tp = lax.axis_size("tp")
    tok_count, width = tokens.shape
    top_count = expert_ids.shape[1]
    experts = n_ep * gate_weight.shape[0]
    capacity = 2 * tok_count * top_count // experts
    if capacity >= tok_count and n_ep == 4 and n_tp == 4 and gate_weight.shape[0] == 1:
        return fused(
            tokens, in_gain, expert_ids, route_weights,
            gate_weight, up_weight, down_weight, out_gain,
        )
    feat_block = width // n_tp
    xf = tokens.astype(jnp.float32)
    normed_in = (
        xf * lax.rsqrt(jnp.mean(xf * xf, axis=1, keepdims=True) + eps) * in_gain.astype(jnp.float32)
    ).astype(jnp.bfloat16)
    flat_ids = expert_ids.reshape(-1)
    onehot = (flat_ids[:, None] == jnp.arange(experts, dtype=jnp.int32)[None, :]).astype(jnp.int32)
    slot = jnp.sum((jnp.cumsum(onehot, axis=0) - onehot) * onehot, axis=1)
    dest = flat_ids * capacity + slot
    token_of = jnp.arange(tok_count * top_count, dtype=jnp.int32) // top_count
    slot_token = jnp.full((experts * capacity,), tok_count, jnp.int32).at[dest].set(token_of)
    source = lax.dynamic_slice_in_dim(normed_in, lax.axis_index("tp") * feat_block, feat_block, 1)
    extended = jnp.concatenate([source, jnp.zeros((1, source.shape[1]), jnp.bfloat16)], axis=0)
    outgoing = extended[slot_token].reshape(experts, capacity, source.shape[1])
    w_gate = gate_weight[0]
    w_up = up_weight[0]
    arrived = lax.all_to_all(outgoing, "ep", split_axis=0, concat_axis=0, tiled=True).reshape(
        n_ep * capacity, feat_block
    )
    piece = lax.all_gather(arrived, "tp", axis=1, tiled=True)
    gate_pre = jnp.dot(piece, w_gate, preferred_element_type=jnp.float32)
    up_pre = jnp.dot(piece, w_up, preferred_element_type=jnp.float32)
    clamped = jnp.minimum(gate_pre, 7.0)
    bounded = jnp.clip(up_pre, -7.0, 7.0)
    act = (clamped * jax.nn.sigmoid(1.702 * clamped) * (bounded + 1.0)).astype(jnp.bfloat16)
    w_down = down_weight[0]
    summed = lax.psum_scatter(
        lax.dot_general(
            w_down, act, (((0,), (1,)), ((), ())), preferred_element_type=jnp.float32
        ).astype(jnp.bfloat16),
        "tp",
        scatter_dimension=0,
        tiled=True,
    )
    summed = summed.reshape(feat_block, n_ep, capacity)
    returned = lax.all_to_all(summed, "ep", split_axis=1, concat_axis=1, tiled=True)
    returned = returned.reshape(feat_block, experts * capacity).T
    picked = returned[dest].astype(jnp.float32).reshape(tok_count, top_count, feat_block)
    combined = jnp.sum(picked * route_weights[:, :, None], axis=1)
    squares = lax.psum(jnp.sum(combined * combined, axis=1), "tp")
    scale = lax.rsqrt(squares / width + eps)
    return (combined * scale[:, None] * out_gain.astype(jnp.float32)).astype(jnp.bfloat16)


def solution(mesh):
    placed = (
        P(("grp", "ep"), None),
        P(),
        P(("grp", "ep"), None),
        P(("grp", "ep"), None),
        P("ep", None, "tp"),
        P("ep", None, "tp"),
        P("ep", "tp", None),
        P("tp"),
    )
    return jax.shard_map(
        on_device, mesh=mesh, in_specs=placed, out_specs=P(("grp", "ep"), "tp"), check_vma=False
    )
```

```python
import jax
import jax.numpy as jnp
from jax import lax
from jax.experimental import pallas as pl
from jax.experimental.pallas import tpu as pltpu
from jax.sharding import PartitionSpec as P

eps = 1e-05
f32 = jnp.float32
bf16 = jnp.bfloat16
pieces = 2
lanes = 128

whole_in = ()
whole_out = (0, 1, )

forwarded = (2, 3)

send_order = (
    (
        (2, 0), (1, 0), (2, 1), (1, 1),
    ),
    (
        (2, 0), (1, 0), (2, 1), (1, 1),
    ),
)

schedules = (
    (
        ("C", 0, 1), ("Z", 1, 0), ("C", 0, 0), ("Z", 1, 1), ("X", 1, 0), ("Z", 3, 0),
        ("C", 1, 0), ("X", 1, 1), ("Z", 2, 0), ("P", 1, 0), ("Q", 1, 0), ("Z", 3, 1),
        ("C", 1, 1), ("X", 2, 0), ("P", 1, 1), ("X", 3, 0), ("Z", 2, 1), ("C", 2, 0),
        ("X", 3, 1), ("P", 2, 0), ("Q", 1, 1), ("C", 3, 0), ("P", 3, 0), ("X", 2, 1),
        ("C", 3, 1), ("Q", 2, 0), ("P", 3, 1), ("C", 2, 1), ("Q", 3, 0), ("P", 2, 1),
        ("Q", 3, 1), ("P", 0, 0), ("P", 0, 1), ("Q", 2, 1), ("Q", 0, 1), ("R", 0, 1),
        ("Q", 0, 0), ("R", 0, 0), ("O", 0, 1), ("O", 0, 0),
    ),
    (
        ("C", 0, 0), ("Z", 3, 0), ("Z", 2, 0), ("Z", 3, 1), ("C", 0, 1), ("X", 2, 0),
        ("Z", 1, 1), ("X", 3, 0), ("Z", 2, 1), ("C", 2, 0), ("X", 3, 1), ("C", 3, 1),
        ("Z", 1, 0), ("P", 2, 0), ("P", 0, 0), ("X", 1, 1), ("C", 3, 0), ("C", 1, 1),
        ("P", 3, 0), ("P", 1, 1), ("Q", 1, 1), ("X", 2, 1), ("P", 3, 1), ("X", 1, 0),
        ("C", 1, 0), ("P", 1, 0), ("C", 2, 1), ("Q", 2, 0), ("Q", 3, 0), ("P", 2, 1),
        ("P", 0, 1), ("Q", 1, 0), ("Q", 3, 1), ("Q", 2, 1), ("Q", 0, 1), ("Q", 0, 0),
        ("R", 0, 0), ("R", 0, 1), ("O", 0, 0), ("O", 0, 1),
    ),
)


def layer_kernel(
    tok, gain_in, ids_in, rw_in, wg, wu, wd, og_in, out,
    gain, ids, rw, og, raw, xbuf, wgu, wdb, g32, table, far_table, share, part, drecv, esend, erecv, brecv, fin,
    mrecv, ret, acc, sq,
    ms, ts, ws, hs, hr, zs, zr, vs, bs, br, ys, yr, xs, xr, ps, pr, ds, dr, es, er, fs, fr, mr, qs, qr,
):
    z, p = lax.axis_index("ep"), lax.axis_index("tp")
    n_ep, n_q, rows, fb = xbuf.shape
    part_rows, hidden = rows // pieces, wg.shape[2]
    half, c = p // 2, p % 2
    mate = half * 2 + 1 - c
    across = (1 - half) * 2 + c
    diagonal = (1 - half) * 2 + 1 - c
    hi = z // 2
    order = (z, 1 - z + hi * 4, 2 - hi, 3 - 3 * hi)
    middle = jnp.logical_or(z == 1, z == 2)

    def span(h):
        return pl.ds(h * part_rows, part_rows)

    def remote(src, dst, s, r, **where):
        return pltpu.make_async_remote_copy(
            src_ref=src, dst_ref=dst, send_sem=s, recv_sem=r,
            device_id=where, device_id_type=pl.DeviceIdType.MESH,
        )

    def signal(**where):
        pl.semaphore_signal(barrier, inc=1, device_id=where, device_id_type=pl.DeviceIdType.MESH)

    loads = [
        [
            pltpu.make_async_copy(
                tok.at[span(h), pl.ds(q * fb, fb)], raw.at[q, span(h)], ts.at[h, q]
            )
            for q in range(n_q)
        ]
        for h in range(pieces)
    ]
    weights = [
        pltpu.make_async_copy(wg.at[0], wgu.at[:, :hidden], ws.at[0]),
        pltpu.make_async_copy(wu.at[0], wgu.at[:, hidden:], ws.at[1]),
    ] + [
        pltpu.make_async_copy(
            wd.at[0, :, pl.ds(q * fb, fb)],
            wdb.at[q % 2, :, pl.ds(q // 2 * fb, fb)], ws.at[2 + q],
        )
        for q in range(n_q)
    ]
    barrier = pltpu.get_barrier_semaphore()
    for peer in (mate, across, diagonal):
        signal(tp=peer)
    for b in order[1:]:
        signal(ep=b)
    small = [
        pltpu.make_async_copy(a, b, ms.at[k])
        for k, (a, b) in enumerate(((gain_in, gain), (ids_in, ids), (rw_in, rw), (og_in, og)))
    ]
    for copy in loads[0] + small + sum(loads[1:], []) + weights:
        copy.start()
    for copy in small:
        copy.wait()
    for q in range(n_q):
        g32[q] = gain[q * (fb // lanes):(q + 1) * (fb // lanes), :].astype(f32)
    for i, e in enumerate(order):
        row = sum(
            jnp.where(ids[k:k + 1, :] == e, rw[k:k + 1, :], 0.0) for k in range(ids.shape[0])
        )
        table[i] = jnp.broadcast_to(row, table.shape[1:])

    def columns(tables):
        rest = jnp.zeros((lanes - 8 * len(tables), rows), f32)
        return jnp.transpose(jnp.concatenate(tables + [rest], axis=0))

    share[0] = columns([table[0]])

    def pipeline(is_middle):
        sends = []

        def push(copy):
            copy.start()
            sends.append(copy)

        def normalize(h):
            for copy in loads[h]:
                copy.wait()
            total = jnp.zeros((part_rows, 1), f32)
            for q in range(n_q):
                v = raw[q, span(h)].astype(f32)
                total += jnp.sum(v * v, axis=1, keepdims=True)
            scale = lax.rsqrt(total / (n_q * fb) + eps)

            def one(q):
                for j in range(fb // lanes):
                    cols = slice(j * lanes, (j + 1) * lanes)
                    g = g32[q][j:j + 1, :]
                    xbuf[z, q, span(h), cols] = (
                        raw[q, span(h), cols].astype(f32) * scale * g
                    ).astype(bf16)

            one(p)
            if h in whole_in:
                one(across)
            if h == 0:
                pl.semaphore_wait(barrier, 6)
                for i in (1, 2, 3):
                    push(remote(table.at[i], far_table.at[z], hs.at[i], hr.at[z], ep=order[i]))
            mine, other = xbuf.at[z, p, span(h)], xbuf.at[z, across, span(h)]
            for i, k in send_order[is_middle]:
                if k == h:
                    push(remote(mine, mine, zs.at[i, h], zr.at[z, h], ep=order[i]))
                    if i == 1 and h in whole_in:
                        push(remote(other, other, ys.at[h], yr.at[h], ep=order[1]))
            for q in (mate, diagonal) if h in whole_in else (across, mate, diagonal):
                one(q)

        def arrived(ref, sem):
            pltpu.make_async_copy(ref, ref, sem).wait()

        def stage_z(i, h):
            b = order[i]
            piece = xbuf.at[b, p, span(h)]
            arrived(piece, zr.at[b, h])
            if i > 1 or h not in whole_in:
                push(remote(piece, piece, xs.at[b, h], xr.at[b, h], tp=across))
            if is_middle and i in forwarded:
                push(remote(piece, piece, vs.at[i, h], zr.at[b, h], ep=order[1]))
            push(remote(piece, piece, ps.at[0, b, h], pr.at[0, b, h], tp=mate))

        def stage_x(i, h):
            b = order[i]
            piece = xbuf.at[b, across, span(h)]
            arrived(piece, yr.at[h] if i == 1 and h in whole_in else xr.at[b, h])
            push(remote(piece, piece, ps.at[1, b, h], pr.at[1, b, h], tp=mate))

        def stage_c(i, h):
            b = order[i]
            if i > 0:
                arrived(xbuf.at[b, mate, span(h)], pr.at[0, b, h])
                arrived(xbuf.at[b, diagonal, span(h)], pr.at[1, b, h])
            if (i, h) == own_first:
                for copy in weights:
                    copy.wait()
            x = jnp.concatenate([xbuf[b, q, span(h)] for q in range(n_q)], axis=1)
            both = jnp.dot(x, wgu[...], preferred_element_type=f32)
            gate = jnp.minimum(both[:, :hidden], 7.0)
            up = jnp.clip(both[:, hidden:], -7.0, 7.0)
            if (i, h) == far_first:
                for e in order[1:]:
                    arrived(far_table.at[e], hr.at[e])
                share[1] = columns([far_table[e] for e in order[1:]])
            k = max(i - 1, 0) * 8
            w = share[min(i, 1), span(h), k:k + 1]
            act = (gate * jax.nn.sigmoid(1.702 * gate) * (up + 1.0) * w).astype(bf16)

            def down(parity):
                y = jnp.dot(act, wdb[parity], preferred_element_type=f32).astype(bf16)
                for k in range(2):
                    part[b, 2 * k + parity, span(h)] = y[:, k * fb:(k + 1) * fb]

            down(1 - c)
            for k in range(2):
                push(remote(
                    part.at[b, 2 * k + 1 - c, span(h)], drecv.at[b, k, span(h)],
                    ds.at[b, k, h], dr.at[b, k, h], tp=mate,
                ))
            down(c)

        def stage_p(i, h):
            b, r = order[i], span(h)
            arrived(drecv.at[b, 1 - half, r], dr.at[b, 1 - half, h])
            value = part[b, across, r].astype(f32) + drecv[b, 1 - half, r].astype(f32)
            if i == 0 and h in whole_out:
                arrived(brecv.at[r], br.at[h])
                value += brecv[r].astype(f32)
            esend[b, r] = value.astype(bf16)
            if i == 1 and h in whole_out:
                push(remote(esend.at[b, r], brecv.at[r], bs.at[h], br.at[h], ep=b))
            else:
                push(remote(esend.at[b, r], erecv.at[b, r], es.at[b, h], er.at[b, h], tp=across))

        def stage_q(i, h):
            b, r = order[i], span(h)
            arrived(drecv.at[b, half, r], dr.at[b, half, h])
            value = part[b, p, r].astype(f32) + drecv[b, half, r].astype(f32)
            if i != 1 or h not in whole_out:
                arrived(erecv.at[b, r], er.at[b, h])
                value += erecv[b, r].astype(f32)
            if i == 0:
                acc[r] = value
                return
            if is_middle and i > 1:
                arrived(mrecv.at[b, r], mr.at[b, h])
                value += mrecv[b, r].astype(f32)
            fin[b, r] = value.astype(bf16)
            if is_middle or i == 1:
                k = min(i, 2) - 1
                push(remote(fin.at[b, r], ret.at[k, r], fs.at[b, h], fr.at[k, h], ep=b))
            else:
                push(remote(fin.at[b, r], mrecv.at[b, r], fs.at[b, h], mr.at[b, h], ep=order[1]))

        def stage_r(i, h):
            r = span(h)
            for k in range(2):
                arrived(ret.at[k, r], fr.at[k, h])
            combined = acc[r] + ret[0, r].astype(f32) + ret[1, r].astype(f32)
            acc[r] = combined
            sums = jnp.sum(combined * combined, axis=1, keepdims=True)
            sq[p, h] = jnp.transpose(jnp.broadcast_to(sums, (part_rows, lanes)))[:8]
            for k, peer in enumerate((mate, across, diagonal)):
                push(remote(sq.at[p, h], sq.at[p, h], qs.at[k, h], qr.at[p, h], tp=peer))

        def stage_o(i, h):
            r = span(h)
            for peer in (mate, across, diagonal):
                arrived(sq.at[peer, h], qr.at[peer, h])
            squares = jnp.transpose(sq[0, h] + sq[1, h] + sq[2, h] + sq[3, h])[:, :1]
            scale = lax.rsqrt(squares / (n_q * fb) + eps)
            og32 = og[...].astype(f32)
            for j in range(fb // lanes):
                cols = slice(j * lanes, (j + 1) * lanes)
                out[r, cols] = (acc[r, cols] * scale * og32[j:j + 1, :]).astype(bf16)

        for h in range(pieces):
            with jax.named_scope(f"N{h}"):
                normalize(h)
        schedule = schedules[is_middle]
        own_first = next(s[1:] for s in schedule if s[0] == "C")
        far_first = next(s[1:] for s in schedule if s[0] == "C" and s[1] > 0)
        stages = {"Z": stage_z, "X": stage_x, "C": stage_c, "P": stage_p, "Q": stage_q}
        stages |= {"R": stage_r, "O": stage_o}
        for name, i, h in schedule:
            with jax.named_scope(f"{name}{i}{h}"):
                stages[name](i, h)
        for copy in sends:
            copy.wait_send()

    pl.when(middle)(lambda: pipeline(True))
    pl.when(jnp.logical_not(middle))(lambda: pipeline(False))


def fused(tokens, in_gain, expert_ids, route_weights, gate_weight, up_weight, down_weight, out_gain):
    n_ep, n_tp = lax.axis_size("ep"), lax.axis_size("tp")
    rows, width = tokens.shape
    hidden = gate_weight.shape[2]
    fb = width // n_tp
    hbm = pl.BlockSpec(memory_space=pl.ANY)
    sem = pltpu.SemaphoreType.DMA
    piece = (rows, fb)
    return pl.pallas_call(
        layer_kernel,
        out_shape=pltpu.VMEM(piece, bf16),
        in_specs=[hbm] * 8,
        out_specs=pl.BlockSpec(memory_space=pltpu.VMEM),
        scratch_shapes=[
            pltpu.VMEM((width // lanes, lanes), bf16),
            pltpu.VMEM(expert_ids.shape[::-1], jnp.int32),
            pltpu.VMEM(route_weights.shape[::-1], f32),
            pltpu.VMEM((fb // lanes, lanes), bf16),
            pltpu.VMEM((n_tp,) + piece, bf16),
            pltpu.VMEM((n_ep, n_tp) + piece, bf16),
            pltpu.VMEM((width, 2 * hidden), bf16),
            pltpu.VMEM((2, hidden, width // 2), bf16),
            pltpu.VMEM((n_tp, fb // lanes, lanes), f32),
            pltpu.VMEM((n_ep, 8, rows), f32),
            pltpu.VMEM((n_ep, 8, rows), f32),
            pltpu.VMEM((2, rows, lanes), f32),
            pltpu.VMEM((n_ep, n_tp) + piece, bf16),
            pltpu.VMEM((n_ep, 2) + piece, bf16),
            pltpu.VMEM((n_ep,) + piece, bf16),
            pltpu.VMEM((n_ep,) + piece, bf16),
            pltpu.VMEM(piece, bf16),
            pltpu.VMEM((n_ep,) + piece, bf16),
            pltpu.VMEM((n_ep,) + piece, bf16),
            pltpu.VMEM((2,) + piece, bf16),
            pltpu.VMEM(piece, f32),
            pltpu.VMEM((n_tp, pieces, 8, rows // pieces), f32),
            sem((4,)), sem((pieces, n_tp)), sem((2 + n_tp,)),
            sem((4,)), sem((n_ep,)),
            sem((4, pieces)), sem((n_ep, pieces)), sem((4, pieces)),
            sem((pieces,)), sem((pieces,)),
            sem((pieces,)), sem((pieces,)),
            sem((n_ep, pieces)), sem((n_ep, pieces)),
            sem((2, n_ep, pieces)), sem((2, n_ep, pieces)),
            sem((n_ep, 2, pieces)), sem((n_ep, 2, pieces)),
            sem((n_ep, pieces)), sem((n_ep, pieces)),
            sem((n_ep, pieces)), sem((2, pieces)), sem((n_ep, pieces)),
            sem((3, pieces)), sem((n_tp, pieces)),
        ],
        compiler_params=pltpu.CompilerParams(
            collective_id=0, has_side_effects=True, vmem_limit_bytes=60 * 1024 * 1024
        ),
        name="layer",
    )(
        tokens, in_gain.reshape(-1, lanes), expert_ids.T, route_weights.T,
        gate_weight, up_weight, down_weight, out_gain.reshape(-1, lanes),
    )


def on_device(
    tokens, in_gain, expert_ids, route_weights, gate_weight, up_weight, down_weight, out_gain
):
    n_ep = lax.axis_size("ep")
    n_tp = lax.axis_size("tp")
    tok_count, width = tokens.shape
    top_count = expert_ids.shape[1]
    experts = n_ep * gate_weight.shape[0]
    capacity = 2 * tok_count * top_count // experts
    if capacity >= tok_count and n_ep == 4 and n_tp == 4 and gate_weight.shape[0] == 1:
        return fused(
            tokens, in_gain, expert_ids, route_weights,
            gate_weight, up_weight, down_weight, out_gain,
        )
    feat_block = width // n_tp
    xf = tokens.astype(jnp.float32)
    normed_in = (
        xf * lax.rsqrt(jnp.mean(xf * xf, axis=1, keepdims=True) + eps) * in_gain.astype(jnp.float32)
    ).astype(jnp.bfloat16)
    flat_ids = expert_ids.reshape(-1)
    onehot = (flat_ids[:, None] == jnp.arange(experts, dtype=jnp.int32)[None, :]).astype(jnp.int32)
    slot = jnp.sum((jnp.cumsum(onehot, axis=0) - onehot) * onehot, axis=1)
    dest = flat_ids * capacity + slot
    token_of = jnp.arange(tok_count * top_count, dtype=jnp.int32) // top_count
    slot_token = jnp.full((experts * capacity,), tok_count, jnp.int32).at[dest].set(token_of)
    source = lax.dynamic_slice_in_dim(normed_in, lax.axis_index("tp") * feat_block, feat_block, 1)
    extended = jnp.concatenate([source, jnp.zeros((1, source.shape[1]), jnp.bfloat16)], axis=0)
    outgoing = extended[slot_token].reshape(experts, capacity, source.shape[1])
    w_gate = gate_weight[0]
    w_up = up_weight[0]
    arrived = lax.all_to_all(outgoing, "ep", split_axis=0, concat_axis=0, tiled=True).reshape(
        n_ep * capacity, feat_block
    )
    piece = lax.all_gather(arrived, "tp", axis=1, tiled=True)
    gate_pre = jnp.dot(piece, w_gate, preferred_element_type=jnp.float32)
    up_pre = jnp.dot(piece, w_up, preferred_element_type=jnp.float32)
    clamped = jnp.minimum(gate_pre, 7.0)
    bounded = jnp.clip(up_pre, -7.0, 7.0)
    act = (clamped * jax.nn.sigmoid(1.702 * clamped) * (bounded + 1.0)).astype(jnp.bfloat16)
    w_down = down_weight[0]
    summed = lax.psum_scatter(
        lax.dot_general(
            w_down, act, (((0,), (1,)), ((), ())), preferred_element_type=jnp.float32
        ).astype(jnp.bfloat16),
        "tp",
        scatter_dimension=0,
        tiled=True,
    )
    summed = summed.reshape(feat_block, n_ep, capacity)
    returned = lax.all_to_all(summed, "ep", split_axis=1, concat_axis=1, tiled=True)
    returned = returned.reshape(feat_block, experts * capacity).T
    picked = returned[dest].astype(jnp.float32).reshape(tok_count, top_count, feat_block)
    combined = jnp.sum(picked * route_weights[:, :, None], axis=1)
    squares = lax.psum(jnp.sum(combined * combined, axis=1), "tp")
    scale = lax.rsqrt(squares / width + eps)
    return (combined * scale[:, None] * out_gain.astype(jnp.float32)).astype(jnp.bfloat16)


def solution(mesh):
    placed = (
        P(("grp", "ep"), None),
        P(),
        P(("grp", "ep"), None),
        P(("grp", "ep"), None),
        P("ep", None, "tp"),
        P("ep", None, "tp"),
        P("ep", "tp", None),
        P("tp"),
    )
    return jax.shard_map(
        on_device, mesh=mesh, in_specs=placed, out_specs=P(("grp", "ep"), "tp"), check_vma=False
    )
```

```python
import jax
import jax.numpy as jnp
from jax import lax
from jax.experimental import pallas as pl
from jax.experimental.pallas import tpu as pltpu
from jax.sharding import PartitionSpec as P

eps = 1e-05
f32 = jnp.float32
bf16 = jnp.bfloat16
pieces = 2
lanes = 128

whole_in = ()
whole_out = (0, 1, )

forwarded = (2, 3)

send_order = (
    (
        (2, 0), (1, 0), (2, 1), (1, 1),
    ),
    (
        (1, 0), (2, 0), (1, 1), (2, 1),
    ),
)

schedules = (
    (
        ("Z", 1, 0), ("Z", 1, 1), ("Z", 3, 0), ("C", 0, 1), ("X", 1, 0), ("X", 1, 1),
        ("Z", 2, 0), ("C", 1, 0), ("Z", 3, 1), ("P", 1, 0), ("X", 3, 0), ("C", 1, 1),
        ("X", 2, 0), ("Q", 1, 0), ("Z", 2, 1), ("C", 2, 0), ("X", 3, 1), ("P", 1, 1),
        ("P", 2, 0), ("C", 3, 0), ("X", 2, 1), ("P", 3, 0), ("C", 3, 1), ("Q", 2, 0),
        ("P", 3, 1), ("C", 2, 1), ("Q", 3, 0), ("P", 2, 1), ("C", 0, 0), ("Q", 3, 1),
        ("P", 0, 0), ("P", 0, 1), ("Q", 2, 1), ("Q", 0, 0), ("R", 0, 0), ("Q", 1, 1),
        ("Q", 0, 1), ("R", 0, 1), ("O", 0, 1), ("O", 0, 0),
    ),
    (
        ("Z", 3, 0), ("C", 0, 0), ("Z", 2, 0), ("Z", 1, 0), ("Z", 3, 1), ("X", 3, 0),
        ("C", 3, 0), ("Z", 2, 1), ("X", 1, 0), ("X", 2, 0), ("C", 1, 0), ("Z", 1, 1),
        ("P", 1, 0), ("C", 2, 0), ("X", 3, 1), ("P", 2, 0), ("C", 0, 1), ("Q", 1, 0),
        ("X", 1, 1), ("P", 3, 0), ("C", 3, 1), ("P", 3, 1), ("X", 2, 1), ("C", 1, 1),
        ("P", 0, 0), ("C", 2, 1), ("P", 1, 1), ("Q", 1, 1), ("Q", 2, 0), ("P", 2, 1),
        ("Q", 3, 0), ("P", 0, 1), ("Q", 0, 0), ("Q", 3, 1), ("R", 0, 0), ("Q", 2, 1),
        ("O", 0, 0), ("Q", 0, 1), ("R", 0, 1), ("O", 0, 1),
    ),
)


def layer_kernel(
    tok, gain_in, ids_in, rw_in, wg, wu, wd, og_in, out,
    gain, ids, rw, og, raw, xbuf, wgu, wdb, g32, table, far_table, share, part, drecv, esend, erecv, brecv, fin,
    mrecv, ret, acc, sq,
    ms, ts, ws, hs, hr, zs, zr, vs, bs, br, ys, yr, xs, xr, ps, pr, ds, dr, es, er, fs, fr, mr, qs, qr,
):
    z, p = lax.axis_index("ep"), lax.axis_index("tp")
    n_ep, n_q, rows, fb = xbuf.shape
    part_rows, hidden = rows // pieces, wg.shape[2]
    half, c = p // 2, p % 2
    mate = half * 2 + 1 - c
    across = (1 - half) * 2 + c
    diagonal = (1 - half) * 2 + 1 - c
    hi = z // 2
    order = (z, 1 - z + hi * 4, 2 - hi, 3 - 3 * hi)
    middle = jnp.logical_or(z == 1, z == 2)

    def span(h):
        return pl.ds(h * part_rows, part_rows)

    def remote(src, dst, s, r, **where):
        return pltpu.make_async_remote_copy(
            src_ref=src, dst_ref=dst, send_sem=s, recv_sem=r,
            device_id=where, device_id_type=pl.DeviceIdType.MESH,
        )

    def signal(**where):
        pl.semaphore_signal(barrier, inc=1, device_id=where, device_id_type=pl.DeviceIdType.MESH)

    loads = [
        [
            pltpu.make_async_copy(
                tok.at[span(h), pl.ds(q * fb, fb)], raw.at[q, span(h)], ts.at[h, q]
            )
            for q in range(n_q)
        ]
        for h in range(pieces)
    ]
    weights = [
        pltpu.make_async_copy(wg.at[0], wgu.at[:, :hidden], ws.at[0]),
        pltpu.make_async_copy(wu.at[0], wgu.at[:, hidden:], ws.at[1]),
    ] + [
        pltpu.make_async_copy(
            wd.at[0, :, pl.ds(q * fb, fb)],
            wdb.at[q % 2, :, pl.ds(q // 2 * fb, fb)], ws.at[2 + q],
        )
        for q in range(n_q)
    ]
    barrier = pltpu.get_barrier_semaphore()
    for peer in (mate, across, diagonal):
        signal(tp=peer)
    for b in order[1:]:
        signal(ep=b)
    small = [
        pltpu.make_async_copy(a, b, ms.at[k])
        for k, (a, b) in enumerate(((gain_in, gain), (ids_in, ids), (rw_in, rw), (og_in, og)))
    ]
    for copy in loads[0] + small + sum(loads[1:], []) + weights:
        copy.start()
    for copy in small:
        copy.wait()
    for q in range(n_q):
        g32[q] = gain[q * (fb // lanes):(q + 1) * (fb // lanes), :].astype(f32)
    for i, e in enumerate(order):
        row = sum(
            jnp.where(ids[k:k + 1, :] == e, rw[k:k + 1, :], 0.0) for k in range(ids.shape[0])
        )
        table[i] = jnp.broadcast_to(row, table.shape[1:])

    def columns(tables):
        rest = jnp.zeros((lanes - 8 * len(tables), rows), f32)
        return jnp.transpose(jnp.concatenate(tables + [rest], axis=0))

    share[0] = columns([table[0]])

    def pipeline(is_middle):
        sends = []

        def push(copy):
            copy.start()
            sends.append(copy)

        def normalize(h):
            for copy in loads[h]:
                copy.wait()
            total = jnp.zeros((part_rows, 1), f32)
            for q in range(n_q):
                v = raw[q, span(h)].astype(f32)
                total += jnp.sum(v * v, axis=1, keepdims=True)
            scale = lax.rsqrt(total / (n_q * fb) + eps)

            def one(q):
                for j in range(fb // lanes):
                    cols = slice(j * lanes, (j + 1) * lanes)
                    g = g32[q][j:j + 1, :]
                    xbuf[z, q, span(h), cols] = (
                        raw[q, span(h), cols].astype(f32) * scale * g
                    ).astype(bf16)

            one(p)
            if h in whole_in:
                one(across)
            if h == 0:
                pl.semaphore_wait(barrier, 6)
                for i in (1, 2, 3):
                    push(remote(table.at[i], far_table.at[z], hs.at[i], hr.at[z], ep=order[i]))
            mine, other = xbuf.at[z, p, span(h)], xbuf.at[z, across, span(h)]
            for i, k in send_order[is_middle]:
                if k == h:
                    push(remote(mine, mine, zs.at[i, h], zr.at[z, h], ep=order[i]))
                    if i == 1 and h in whole_in:
                        push(remote(other, other, ys.at[h], yr.at[h], ep=order[1]))
            for q in (mate, diagonal) if h in whole_in else (across, mate, diagonal):
                one(q)

        def arrived(ref, sem):
            pltpu.make_async_copy(ref, ref, sem).wait()

        def stage_z(i, h):
            b = order[i]
            piece = xbuf.at[b, p, span(h)]
            arrived(piece, zr.at[b, h])
            if i > 1 or h not in whole_in:
                push(remote(piece, piece, xs.at[b, h], xr.at[b, h], tp=across))
            if is_middle and i in forwarded:
                push(remote(piece, piece, vs.at[i, h], zr.at[b, h], ep=order[1]))
            push(remote(piece, piece, ps.at[0, b, h], pr.at[0, b, h], tp=mate))

        def stage_x(i, h):
            b = order[i]
            piece = xbuf.at[b, across, span(h)]
            arrived(piece, yr.at[h] if i == 1 and h in whole_in else xr.at[b, h])
            push(remote(piece, piece, ps.at[1, b, h], pr.at[1, b, h], tp=mate))

        def stage_c(i, h):
            b = order[i]
            if i > 0:
                arrived(xbuf.at[b, mate, span(h)], pr.at[0, b, h])
                arrived(xbuf.at[b, diagonal, span(h)], pr.at[1, b, h])
            if (i, h) == own_first:
                for copy in weights:
                    copy.wait()
            x = jnp.concatenate([xbuf[b, q, span(h)] for q in range(n_q)], axis=1)
            both = jnp.dot(x, wgu[...], preferred_element_type=f32)
            gate = jnp.minimum(both[:, :hidden], 7.0)
            up = jnp.clip(both[:, hidden:], -7.0, 7.0)
            if (i, h) == far_first:
                for e in order[1:]:
                    arrived(far_table.at[e], hr.at[e])
                share[1] = columns([far_table[e] for e in order[1:]])
            k = max(i - 1, 0) * 8
            w = share[min(i, 1), span(h), k:k + 1]
            act = (gate * jax.nn.sigmoid(1.702 * gate) * (up + 1.0) * w).astype(bf16)

            def down(parity):
                y = jnp.dot(act, wdb[parity], preferred_element_type=f32).astype(bf16)
                for k in range(2):
                    part[b, 2 * k + parity, span(h)] = y[:, k * fb:(k + 1) * fb]

            down(1 - c)
            for k in range(2):
                push(remote(
                    part.at[b, 2 * k + 1 - c, span(h)], drecv.at[b, k, span(h)],
                    ds.at[b, k, h], dr.at[b, k, h], tp=mate,
                ))
            down(c)

        def stage_p(i, h):
            b, r = order[i], span(h)
            arrived(drecv.at[b, 1 - half, r], dr.at[b, 1 - half, h])
            value = part[b, across, r].astype(f32) + drecv[b, 1 - half, r].astype(f32)
            if i == 0 and h in whole_out:
                arrived(brecv.at[r], br.at[h])
                value += brecv[r].astype(f32)
            esend[b, r] = value.astype(bf16)
            if i == 1 and h in whole_out:
                push(remote(esend.at[b, r], brecv.at[r], bs.at[h], br.at[h], ep=b))
            else:
                push(remote(esend.at[b, r], erecv.at[b, r], es.at[b, h], er.at[b, h], tp=across))

        def stage_q(i, h):
            b, r = order[i], span(h)
            arrived(drecv.at[b, half, r], dr.at[b, half, h])
            value = part[b, p, r].astype(f32) + drecv[b, half, r].astype(f32)
            if i != 1 or h not in whole_out:
                arrived(erecv.at[b, r], er.at[b, h])
                value += erecv[b, r].astype(f32)
            if i == 0:
                acc[r] = value
                return
            if is_middle and i > 1:
                arrived(mrecv.at[b, r], mr.at[b, h])
                value += mrecv[b, r].astype(f32)
            fin[b, r] = value.astype(bf16)
            if is_middle or i == 1:
                k = min(i, 2) - 1
                push(remote(fin.at[b, r], ret.at[k, r], fs.at[b, h], fr.at[k, h], ep=b))
            else:
                push(remote(fin.at[b, r], mrecv.at[b, r], fs.at[b, h], mr.at[b, h], ep=order[1]))

        def stage_r(i, h):
            r = span(h)
            for k in range(2):
                arrived(ret.at[k, r], fr.at[k, h])
            combined = acc[r] + ret[0, r].astype(f32) + ret[1, r].astype(f32)
            acc[r] = combined
            sums = jnp.sum(combined * combined, axis=1, keepdims=True)
            sq[p, h] = jnp.transpose(jnp.broadcast_to(sums, (part_rows, lanes)))[:8]
            for k, peer in enumerate((mate, across, diagonal)):
                push(remote(sq.at[p, h], sq.at[p, h], qs.at[k, h], qr.at[p, h], tp=peer))

        def stage_o(i, h):
            r = span(h)
            for peer in (mate, across, diagonal):
                arrived(sq.at[peer, h], qr.at[peer, h])
            squares = jnp.transpose(sq[0, h] + sq[1, h] + sq[2, h] + sq[3, h])[:, :1]
            scale = lax.rsqrt(squares / (n_q * fb) + eps)
            og32 = og[...].astype(f32)
            for j in range(fb // lanes):
                cols = slice(j * lanes, (j + 1) * lanes)
                out[r, cols] = (acc[r, cols] * scale * og32[j:j + 1, :]).astype(bf16)

        for h in range(pieces):
            with jax.named_scope(f"N{h}"):
                normalize(h)
        schedule = schedules[is_middle]
        own_first = next(s[1:] for s in schedule if s[0] == "C")
        far_first = next(s[1:] for s in schedule if s[0] == "C" and s[1] > 0)
        stages = {"Z": stage_z, "X": stage_x, "C": stage_c, "P": stage_p, "Q": stage_q}
        stages |= {"R": stage_r, "O": stage_o}
        for name, i, h in schedule:
            with jax.named_scope(f"{name}{i}{h}"):
                stages[name](i, h)
        for copy in sends:
            copy.wait_send()

    pl.when(middle)(lambda: pipeline(True))
    pl.when(jnp.logical_not(middle))(lambda: pipeline(False))


def fused(tokens, in_gain, expert_ids, route_weights, gate_weight, up_weight, down_weight, out_gain):
    n_ep, n_tp = lax.axis_size("ep"), lax.axis_size("tp")
    rows, width = tokens.shape
    hidden = gate_weight.shape[2]
    fb = width // n_tp
    hbm = pl.BlockSpec(memory_space=pl.ANY)
    sem = pltpu.SemaphoreType.DMA
    piece = (rows, fb)
    return pl.pallas_call(
        layer_kernel,
        out_shape=pltpu.VMEM(piece, bf16),
        in_specs=[hbm] * 8,
        out_specs=pl.BlockSpec(memory_space=pltpu.VMEM),
        scratch_shapes=[
            pltpu.VMEM((width // lanes, lanes), bf16),
            pltpu.VMEM(expert_ids.shape[::-1], jnp.int32),
            pltpu.VMEM(route_weights.shape[::-1], f32),
            pltpu.VMEM((fb // lanes, lanes), bf16),
            pltpu.VMEM((n_tp,) + piece, bf16),
            pltpu.VMEM((n_ep, n_tp) + piece, bf16),
            pltpu.VMEM((width, 2 * hidden), bf16),
            pltpu.VMEM((2, hidden, width // 2), bf16),
            pltpu.VMEM((n_tp, fb // lanes, lanes), f32),
            pltpu.VMEM((n_ep, 8, rows), f32),
            pltpu.VMEM((n_ep, 8, rows), f32),
            pltpu.VMEM((2, rows, lanes), f32),
            pltpu.VMEM((n_ep, n_tp) + piece, bf16),
            pltpu.VMEM((n_ep, 2) + piece, bf16),
            pltpu.VMEM((n_ep,) + piece, bf16),
            pltpu.VMEM((n_ep,) + piece, bf16),
            pltpu.VMEM(piece, bf16),
            pltpu.VMEM((n_ep,) + piece, bf16),
            pltpu.VMEM((n_ep,) + piece, bf16),
            pltpu.VMEM((2,) + piece, bf16),
            pltpu.VMEM(piece, f32),
            pltpu.VMEM((n_tp, pieces, 8, rows // pieces), f32),
            sem((4,)), sem((pieces, n_tp)), sem((2 + n_tp,)),
            sem((4,)), sem((n_ep,)),
            sem((4, pieces)), sem((n_ep, pieces)), sem((4, pieces)),
            sem((pieces,)), sem((pieces,)),
            sem((pieces,)), sem((pieces,)),
            sem((n_ep, pieces)), sem((n_ep, pieces)),
            sem((2, n_ep, pieces)), sem((2, n_ep, pieces)),
            sem((n_ep, 2, pieces)), sem((n_ep, 2, pieces)),
            sem((n_ep, pieces)), sem((n_ep, pieces)),
            sem((n_ep, pieces)), sem((2, pieces)), sem((n_ep, pieces)),
            sem((3, pieces)), sem((n_tp, pieces)),
        ],
        compiler_params=pltpu.CompilerParams(
            collective_id=0, has_side_effects=True, vmem_limit_bytes=60 * 1024 * 1024
        ),
        name="layer",
    )(
        tokens, in_gain.reshape(-1, lanes), expert_ids.T, route_weights.T,
        gate_weight, up_weight, down_weight, out_gain.reshape(-1, lanes),
    )


def on_device(
    tokens, in_gain, expert_ids, route_weights, gate_weight, up_weight, down_weight, out_gain
):
    n_ep = lax.axis_size("ep")
    n_tp = lax.axis_size("tp")
    tok_count, width = tokens.shape
    top_count = expert_ids.shape[1]
    experts = n_ep * gate_weight.shape[0]
    capacity = 2 * tok_count * top_count // experts
    if capacity >= tok_count and n_ep == 4 and n_tp == 4 and gate_weight.shape[0] == 1:
        return fused(
            tokens, in_gain, expert_ids, route_weights,
            gate_weight, up_weight, down_weight, out_gain,
        )
    feat_block = width // n_tp
    xf = tokens.astype(jnp.float32)
    normed_in = (
        xf * lax.rsqrt(jnp.mean(xf * xf, axis=1, keepdims=True) + eps) * in_gain.astype(jnp.float32)
    ).astype(jnp.bfloat16)
    flat_ids = expert_ids.reshape(-1)
    onehot = (flat_ids[:, None] == jnp.arange(experts, dtype=jnp.int32)[None, :]).astype(jnp.int32)
    slot = jnp.sum((jnp.cumsum(onehot, axis=0) - onehot) * onehot, axis=1)
    dest = flat_ids * capacity + slot
    token_of = jnp.arange(tok_count * top_count, dtype=jnp.int32) // top_count
    slot_token = jnp.full((experts * capacity,), tok_count, jnp.int32).at[dest].set(token_of)
    source = lax.dynamic_slice_in_dim(normed_in, lax.axis_index("tp") * feat_block, feat_block, 1)
    extended = jnp.concatenate([source, jnp.zeros((1, source.shape[1]), jnp.bfloat16)], axis=0)
    outgoing = extended[slot_token].reshape(experts, capacity, source.shape[1])
    w_gate = gate_weight[0]
    w_up = up_weight[0]
    arrived = lax.all_to_all(outgoing, "ep", split_axis=0, concat_axis=0, tiled=True).reshape(
        n_ep * capacity, feat_block
    )
    piece = lax.all_gather(arrived, "tp", axis=1, tiled=True)
    gate_pre = jnp.dot(piece, w_gate, preferred_element_type=jnp.float32)
    up_pre = jnp.dot(piece, w_up, preferred_element_type=jnp.float32)
    clamped = jnp.minimum(gate_pre, 7.0)
    bounded = jnp.clip(up_pre, -7.0, 7.0)
    act = (clamped * jax.nn.sigmoid(1.702 * clamped) * (bounded + 1.0)).astype(jnp.bfloat16)
    w_down = down_weight[0]
    summed = lax.psum_scatter(
        lax.dot_general(
            w_down, act, (((0,), (1,)), ((), ())), preferred_element_type=jnp.float32
        ).astype(jnp.bfloat16),
        "tp",
        scatter_dimension=0,
        tiled=True,
    )
    summed = summed.reshape(feat_block, n_ep, capacity)
    returned = lax.all_to_all(summed, "ep", split_axis=1, concat_axis=1, tiled=True)
    returned = returned.reshape(feat_block, experts * capacity).T
    picked = returned[dest].astype(jnp.float32).reshape(tok_count, top_count, feat_block)
    combined = jnp.sum(picked * route_weights[:, :, None], axis=1)
    squares = lax.psum(jnp.sum(combined * combined, axis=1), "tp")
    scale = lax.rsqrt(squares / width + eps)
    return (combined * scale[:, None] * out_gain.astype(jnp.float32)).astype(jnp.bfloat16)


def solution(mesh):
    placed = (
        P(("grp", "ep"), None),
        P(),
        P(("grp", "ep"), None),
        P(("grp", "ep"), None),
        P("ep", None, "tp"),
        P("ep", None, "tp"),
        P("ep", "tp", None),
        P("tp"),
    )
    return jax.shard_map(
        on_device, mesh=mesh, in_specs=placed, out_specs=P(("grp", "ep"), "tp"), check_vma=False
    )
```

```python
import jax
import jax.numpy as jnp
from jax import lax
from jax.experimental import pallas as pl
from jax.experimental.pallas import tpu as pltpu
from jax.sharding import PartitionSpec as P

eps = 1e-05
f32 = jnp.float32
bf16 = jnp.bfloat16
pieces = 2
lanes = 128

whole_in = ()
whole_out = (0, 1, )

forwarded = (2, 3)

send_order = (
    (
        (2, 0), (1, 0), (2, 1), (1, 1),
    ),
    (
        (1, 0), (2, 0), (1, 1), (2, 1),
    ),
)

schedules = (
    (
        ("Z", 1, 0), ("Z", 1, 1), ("Z", 3, 0), ("C", 0, 1), ("X", 1, 0), ("X", 1, 1),
        ("Z", 2, 0), ("C", 1, 0), ("Z", 3, 1), ("P", 1, 0), ("X", 3, 0), ("C", 1, 1),
        ("X", 2, 0), ("Q", 1, 0), ("Z", 2, 1), ("C", 2, 0), ("X", 3, 1), ("P", 1, 1),
        ("P", 2, 0), ("C", 3, 0), ("X", 2, 1), ("P", 3, 0), ("C", 3, 1), ("Q", 2, 0),
        ("P", 3, 1), ("C", 2, 1), ("Q", 3, 0), ("P", 2, 1), ("C", 0, 0), ("Q", 3, 1),
        ("P", 0, 0), ("P", 0, 1), ("Q", 2, 1), ("Q", 0, 0), ("R", 0, 0), ("Q", 1, 1),
        ("Q", 0, 1), ("R", 0, 1), ("O", 0, 1), ("O", 0, 0),
    ),
    (
        ("Z", 3, 0), ("C", 0, 0), ("Z", 2, 0), ("Z", 1, 0), ("Z", 3, 1), ("X", 3, 0),
        ("C", 3, 0), ("Z", 2, 1), ("X", 1, 0), ("X", 2, 0), ("C", 1, 0), ("Z", 1, 1),
        ("P", 1, 0), ("C", 2, 0), ("X", 3, 1), ("P", 2, 0), ("C", 0, 1), ("Q", 1, 0),
        ("X", 1, 1), ("P", 3, 0), ("C", 3, 1), ("P", 3, 1), ("X", 2, 1), ("C", 1, 1),
        ("P", 0, 0), ("C", 2, 1), ("P", 1, 1), ("Q", 1, 1), ("Q", 2, 0), ("P", 2, 1),
        ("Q", 3, 0), ("P", 0, 1), ("Q", 0, 0), ("Q", 3, 1), ("R", 0, 0), ("Q", 2, 1),
        ("O", 0, 0), ("Q", 0, 1), ("R", 0, 1), ("O", 0, 1),
    ),
)


def layer_kernel(
    tok, gain_in, ids_in, rw_in, wg, wu, wd, og_in, out,
    gain, ids, rw, og, raw, xbuf, wgu, wdb, g32, table, far_table, share, part, drecv, esend, erecv, brecv, fin,
    mrecv, ret, acc, sq,
    ms, ts, ws, hs, hr, zs, zr, vs, bs, br, ys, yr, xs, xr, ps, pr, ds, dr, es, er, fs, fr, mr, qs, qr,
):
    z, p = lax.axis_index("ep"), lax.axis_index("tp")
    n_ep, n_q, rows, fb = xbuf.shape
    part_rows, hidden = rows // pieces, wg.shape[2]
    half, c = p // 2, p % 2
    mate = half * 2 + 1 - c
    across = (1 - half) * 2 + c
    diagonal = (1 - half) * 2 + 1 - c
    hi = z // 2
    order = (z, 1 - z + hi * 4, 2 - hi, 3 - 3 * hi)
    middle = jnp.logical_or(z == 1, z == 2)

    def span(h):
        return pl.ds(h * part_rows, part_rows)

    def remote(src, dst, s, r, **where):
        return pltpu.make_async_remote_copy(
            src_ref=src, dst_ref=dst, send_sem=s, recv_sem=r,
            device_id=where, device_id_type=pl.DeviceIdType.MESH,
        )

    def signal(**where):
        pl.semaphore_signal(barrier, inc=1, device_id=where, device_id_type=pl.DeviceIdType.MESH)

    loads = [
        [
            pltpu.make_async_copy(
                tok.at[span(h), pl.ds(q * fb, fb)], raw.at[q, span(h)], ts.at[h, q]
            )
            for q in range(n_q)
        ]
        for h in range(pieces)
    ]
    weights = [
        pltpu.make_async_copy(wg.at[0], wgu.at[:, :hidden], ws.at[0]),
        pltpu.make_async_copy(wu.at[0], wgu.at[:, hidden:], ws.at[1]),
    ] + [
        pltpu.make_async_copy(
            wd.at[0, :, pl.ds(q * fb, fb)],
            wdb.at[q % 2, :, pl.ds(q // 2 * fb, fb)], ws.at[2 + q],
        )
        for q in range(n_q)
    ]
    barrier = pltpu.get_barrier_semaphore()
    for peer in (mate, across, diagonal):
        signal(tp=peer)
    for b in order[1:]:
        signal(ep=b)
    small = [
        pltpu.make_async_copy(a, b, ms.at[k])
        for k, (a, b) in enumerate(((gain_in, gain), (ids_in, ids), (rw_in, rw), (og_in, og)))
    ]
    for copy in loads[0] + small + sum(loads[1:], []) + weights:
        copy.start()
    for copy in small:
        copy.wait()
    for q in range(n_q):
        g32[q] = gain[q * (fb // lanes):(q + 1) * (fb // lanes), :].astype(f32)
    for i, e in enumerate(order):
        row = sum(
            jnp.where(ids[k:k + 1, :] == e, rw[k:k + 1, :], 0.0) for k in range(ids.shape[0])
        )
        table[i] = jnp.broadcast_to(row, table.shape[1:])

    def columns(tables):
        rest = jnp.zeros((lanes - 8 * len(tables), rows), f32)
        return jnp.transpose(jnp.concatenate(tables + [rest], axis=0))

    share[0] = columns([table[0]])

    def pipeline(is_middle):
        sends = []

        def push(copy):
            copy.start()
            sends.append(copy)

        def normalize(h):
            for copy in loads[h]:
                copy.wait()
            total = jnp.zeros((part_rows, 1), f32)
            for q in range(n_q):
                v = raw[q, span(h)].astype(f32)
                total += jnp.sum(v * v, axis=1, keepdims=True)
            scale = lax.rsqrt(total / (n_q * fb) + eps)

            def one(q):
                for j in range(fb // lanes):
                    cols = slice(j * lanes, (j + 1) * lanes)
                    g = g32[q][j:j + 1, :]
                    xbuf[z, q, span(h), cols] = (
                        raw[q, span(h), cols].astype(f32) * scale * g
                    ).astype(bf16)

            one(p)
            if h in whole_in:
                one(across)
            if h == 0:
                pl.semaphore_wait(barrier, 6)
            mine, other = xbuf.at[z, p, span(h)], xbuf.at[z, across, span(h)]
            for i, k in send_order[is_middle]:
                if k == h:
                    push(remote(mine, mine, zs.at[i, h], zr.at[z, h], ep=order[i]))
                    if i == 1 and h in whole_in:
                        push(remote(other, other, ys.at[h], yr.at[h], ep=order[1]))
            if h == 0:
                for i in (1, 2, 3):
                    push(remote(table.at[i], far_table.at[z], hs.at[i], hr.at[z], ep=order[i]))
            for q in (mate, diagonal) if h in whole_in else (across, mate, diagonal):
                one(q)

        def arrived(ref, sem):
            pltpu.make_async_copy(ref, ref, sem).wait()

        def stage_z(i, h):
            b = order[i]
            piece = xbuf.at[b, p, span(h)]
            arrived(piece, zr.at[b, h])
            if i > 1 or h not in whole_in:
                push(remote(piece, piece, xs.at[b, h], xr.at[b, h], tp=across))
            if is_middle and i in forwarded:
                push(remote(piece, piece, vs.at[i, h], zr.at[b, h], ep=order[1]))
            push(remote(piece, piece, ps.at[0, b, h], pr.at[0, b, h], tp=mate))

        def stage_x(i, h):
            b = order[i]
            piece = xbuf.at[b, across, span(h)]
            arrived(piece, yr.at[h] if i == 1 and h in whole_in else xr.at[b, h])
            push(remote(piece, piece, ps.at[1, b, h], pr.at[1, b, h], tp=mate))

        def stage_c(i, h):
            b = order[i]
            if i > 0:
                arrived(xbuf.at[b, mate, span(h)], pr.at[0, b, h])
                arrived(xbuf.at[b, diagonal, span(h)], pr.at[1, b, h])
            if (i, h) == own_first:
                for copy in weights:
                    copy.wait()
            x = jnp.concatenate([xbuf[b, q, span(h)] for q in range(n_q)], axis=1)
            both = jnp.dot(x, wgu[...], preferred_element_type=f32)
            gate = jnp.minimum(both[:, :hidden], 7.0)
            up = jnp.clip(both[:, hidden:], -7.0, 7.0)
            if (i, h) == far_first:
                for e in order[1:]:
                    arrived(far_table.at[e], hr.at[e])
                share[1] = columns([far_table[e] for e in order[1:]])
            k = max(i - 1, 0) * 8
            w = share[min(i, 1), span(h), k:k + 1]
            act = (gate * jax.nn.sigmoid(1.702 * gate) * (up + 1.0) * w).astype(bf16)

            def down(parity):
                y = jnp.dot(act, wdb[parity], preferred_element_type=f32).astype(bf16)
                for k in range(2):
                    part[b, 2 * k + parity, span(h)] = y[:, k * fb:(k + 1) * fb]

            down(1 - c)
            for k in range(2):
                push(remote(
                    part.at[b, 2 * k + 1 - c, span(h)], drecv.at[b, k, span(h)],
                    ds.at[b, k, h], dr.at[b, k, h], tp=mate,
                ))
            down(c)

        def stage_p(i, h):
            b, r = order[i], span(h)
            arrived(drecv.at[b, 1 - half, r], dr.at[b, 1 - half, h])
            value = part[b, across, r].astype(f32) + drecv[b, 1 - half, r].astype(f32)
            if i == 0 and h in whole_out:
                arrived(brecv.at[r], br.at[h])
                value += brecv[r].astype(f32)
            esend[b, r] = value.astype(bf16)
            if i == 1 and h in whole_out:
                push(remote(esend.at[b, r], brecv.at[r], bs.at[h], br.at[h], ep=b))
            else:
                push(remote(esend.at[b, r], erecv.at[b, r], es.at[b, h], er.at[b, h], tp=across))

        def stage_q(i, h):
            b, r = order[i], span(h)
            arrived(drecv.at[b, half, r], dr.at[b, half, h])
            value = part[b, p, r].astype(f32) + drecv[b, half, r].astype(f32)
            if i != 1 or h not in whole_out:
                arrived(erecv.at[b, r], er.at[b, h])
                value += erecv[b, r].astype(f32)
            if i == 0:
                acc[r] = value
                return
            if is_middle and i > 1:
                arrived(mrecv.at[b, r], mr.at[b, h])
                value += mrecv[b, r].astype(f32)
            fin[b, r] = value.astype(bf16)
            if is_middle or i == 1:
                k = min(i, 2) - 1
                push(remote(fin.at[b, r], ret.at[k, r], fs.at[b, h], fr.at[k, h], ep=b))
            else:
                push(remote(fin.at[b, r], mrecv.at[b, r], fs.at[b, h], mr.at[b, h], ep=order[1]))

        def stage_r(i, h):
            r = span(h)
            for k in range(2):
                arrived(ret.at[k, r], fr.at[k, h])
            combined = acc[r] + ret[0, r].astype(f32) + ret[1, r].astype(f32)
            acc[r] = combined
            sums = jnp.sum(combined * combined, axis=1, keepdims=True)
            sq[p, h] = jnp.transpose(jnp.broadcast_to(sums, (part_rows, lanes)))[:8]
            for k, peer in enumerate((mate, across, diagonal)):
                push(remote(sq.at[p, h], sq.at[p, h], qs.at[k, h], qr.at[p, h], tp=peer))

        def stage_o(i, h):
            r = span(h)
            for peer in (mate, across, diagonal):
                arrived(sq.at[peer, h], qr.at[peer, h])
            squares = jnp.transpose(sq[0, h] + sq[1, h] + sq[2, h] + sq[3, h])[:, :1]
            scale = lax.rsqrt(squares / (n_q * fb) + eps)
            og32 = og[...].astype(f32)
            for j in range(fb // lanes):
                cols = slice(j * lanes, (j + 1) * lanes)
                out[r, cols] = (acc[r, cols] * scale * og32[j:j + 1, :]).astype(bf16)

        for h in range(pieces):
            with jax.named_scope(f"N{h}"):
                normalize(h)
        schedule = schedules[is_middle]
        own_first = next(s[1:] for s in schedule if s[0] == "C")
        far_first = next(s[1:] for s in schedule if s[0] == "C" and s[1] > 0)
        stages = {"Z": stage_z, "X": stage_x, "C": stage_c, "P": stage_p, "Q": stage_q}
        stages |= {"R": stage_r, "O": stage_o}
        for name, i, h in schedule:
            with jax.named_scope(f"{name}{i}{h}"):
                stages[name](i, h)
        for copy in sends:
            copy.wait_send()

    pl.when(middle)(lambda: pipeline(True))
    pl.when(jnp.logical_not(middle))(lambda: pipeline(False))


def fused(tokens, in_gain, expert_ids, route_weights, gate_weight, up_weight, down_weight, out_gain):
    n_ep, n_tp = lax.axis_size("ep"), lax.axis_size("tp")
    rows, width = tokens.shape
    hidden = gate_weight.shape[2]
    fb = width // n_tp
    hbm = pl.BlockSpec(memory_space=pl.ANY)
    sem = pltpu.SemaphoreType.DMA
    piece = (rows, fb)
    return pl.pallas_call(
        layer_kernel,
        out_shape=pltpu.VMEM(piece, bf16),
        in_specs=[hbm] * 8,
        out_specs=pl.BlockSpec(memory_space=pltpu.VMEM),
        scratch_shapes=[
            pltpu.VMEM((width // lanes, lanes), bf16),
            pltpu.VMEM(expert_ids.shape[::-1], jnp.int32),
            pltpu.VMEM(route_weights.shape[::-1], f32),
            pltpu.VMEM((fb // lanes, lanes), bf16),
            pltpu.VMEM((n_tp,) + piece, bf16),
            pltpu.VMEM((n_ep, n_tp) + piece, bf16),
            pltpu.VMEM((width, 2 * hidden), bf16),
            pltpu.VMEM((2, hidden, width // 2), bf16),
            pltpu.VMEM((n_tp, fb // lanes, lanes), f32),
            pltpu.VMEM((n_ep, 8, rows), f32),
            pltpu.VMEM((n_ep, 8, rows), f32),
            pltpu.VMEM((2, rows, lanes), f32),
            pltpu.VMEM((n_ep, n_tp) + piece, bf16),
            pltpu.VMEM((n_ep, 2) + piece, bf16),
            pltpu.VMEM((n_ep,) + piece, bf16),
            pltpu.VMEM((n_ep,) + piece, bf16),
            pltpu.VMEM(piece, bf16),
            pltpu.VMEM((n_ep,) + piece, bf16),
            pltpu.VMEM((n_ep,) + piece, bf16),
            pltpu.VMEM((2,) + piece, bf16),
            pltpu.VMEM(piece, f32),
            pltpu.VMEM((n_tp, pieces, 8, rows // pieces), f32),
            sem((4,)), sem((pieces, n_tp)), sem((2 + n_tp,)),
            sem((4,)), sem((n_ep,)),
            sem((4, pieces)), sem((n_ep, pieces)), sem((4, pieces)),
            sem((pieces,)), sem((pieces,)),
            sem((pieces,)), sem((pieces,)),
            sem((n_ep, pieces)), sem((n_ep, pieces)),
            sem((2, n_ep, pieces)), sem((2, n_ep, pieces)),
            sem((n_ep, 2, pieces)), sem((n_ep, 2, pieces)),
            sem((n_ep, pieces)), sem((n_ep, pieces)),
            sem((n_ep, pieces)), sem((2, pieces)), sem((n_ep, pieces)),
            sem((3, pieces)), sem((n_tp, pieces)),
        ],
        compiler_params=pltpu.CompilerParams(
            collective_id=0, has_side_effects=True, vmem_limit_bytes=60 * 1024 * 1024
        ),
        name="layer",
    )(
        tokens, in_gain.reshape(-1, lanes), expert_ids.T, route_weights.T,
        gate_weight, up_weight, down_weight, out_gain.reshape(-1, lanes),
    )


def on_device(
    tokens, in_gain, expert_ids, route_weights, gate_weight, up_weight, down_weight, out_gain
):
    n_ep = lax.axis_size("ep")
    n_tp = lax.axis_size("tp")
    tok_count, width = tokens.shape
    top_count = expert_ids.shape[1]
    experts = n_ep * gate_weight.shape[0]
    capacity = 2 * tok_count * top_count // experts
    if capacity >= tok_count and n_ep == 4 and n_tp == 4 and gate_weight.shape[0] == 1:
        return fused(
            tokens, in_gain, expert_ids, route_weights,
            gate_weight, up_weight, down_weight, out_gain,
        )
    feat_block = width // n_tp
    xf = tokens.astype(jnp.float32)
    normed_in = (
        xf * lax.rsqrt(jnp.mean(xf * xf, axis=1, keepdims=True) + eps) * in_gain.astype(jnp.float32)
    ).astype(jnp.bfloat16)
    flat_ids = expert_ids.reshape(-1)
    onehot = (flat_ids[:, None] == jnp.arange(experts, dtype=jnp.int32)[None, :]).astype(jnp.int32)
    slot = jnp.sum((jnp.cumsum(onehot, axis=0) - onehot) * onehot, axis=1)
    dest = flat_ids * capacity + slot
    token_of = jnp.arange(tok_count * top_count, dtype=jnp.int32) // top_count
    slot_token = jnp.full((experts * capacity,), tok_count, jnp.int32).at[dest].set(token_of)
    source = lax.dynamic_slice_in_dim(normed_in, lax.axis_index("tp") * feat_block, feat_block, 1)
    extended = jnp.concatenate([source, jnp.zeros((1, source.shape[1]), jnp.bfloat16)], axis=0)
    outgoing = extended[slot_token].reshape(experts, capacity, source.shape[1])
    w_gate = gate_weight[0]
    w_up = up_weight[0]
    arrived = lax.all_to_all(outgoing, "ep", split_axis=0, concat_axis=0, tiled=True).reshape(
        n_ep * capacity, feat_block
    )
    piece = lax.all_gather(arrived, "tp", axis=1, tiled=True)
    gate_pre = jnp.dot(piece, w_gate, preferred_element_type=jnp.float32)
    up_pre = jnp.dot(piece, w_up, preferred_element_type=jnp.float32)
    clamped = jnp.minimum(gate_pre, 7.0)
    bounded = jnp.clip(up_pre, -7.0, 7.0)
    act = (clamped * jax.nn.sigmoid(1.702 * clamped) * (bounded + 1.0)).astype(jnp.bfloat16)
    w_down = down_weight[0]
    summed = lax.psum_scatter(
        lax.dot_general(
            w_down, act, (((0,), (1,)), ((), ())), preferred_element_type=jnp.float32
        ).astype(jnp.bfloat16),
        "tp",
        scatter_dimension=0,
        tiled=True,
    )
    summed = summed.reshape(feat_block, n_ep, capacity)
    returned = lax.all_to_all(summed, "ep", split_axis=1, concat_axis=1, tiled=True)
    returned = returned.reshape(feat_block, experts * capacity).T
    picked = returned[dest].astype(jnp.float32).reshape(tok_count, top_count, feat_block)
    combined = jnp.sum(picked * route_weights[:, :, None], axis=1)
    squares = lax.psum(jnp.sum(combined * combined, axis=1), "tp")
    scale = lax.rsqrt(squares / width + eps)
    return (combined * scale[:, None] * out_gain.astype(jnp.float32)).astype(jnp.bfloat16)


def solution(mesh):
    placed = (
        P(("grp", "ep"), None),
        P(),
        P(("grp", "ep"), None),
        P(("grp", "ep"), None),
        P("ep", None, "tp"),
        P("ep", None, "tp"),
        P("ep", "tp", None),
        P("tp"),
    )
    return jax.shard_map(
        on_device, mesh=mesh, in_specs=placed, out_specs=P(("grp", "ep"), "tp"), check_vma=False
    )
```
